256 devices in a mesh: grp: 2 (over y), sp: 16 (over z), tp: 8 (over x, core).
Axes of the slice: x: 4, y: 2, z: 16, core: 2. Of those that a mesh axis runs over, the one named last changes fastest.
The devices are a block of a 4x16x16 slice.
Arguments:
- latent: bfloat16 [8192, 2048], P(('grp', 'sp', 'tp')), parts along dimension 0, may hold values from -6 to 6
- cond: bfloat16 [4096], P(('grp', 'sp')), parts along dimension 0, may hold values from -6 to 6
- context: bfloat16 [2048, 2048], P(('grp', 'sp')), parts along dimension 0, may hold values from -6 to 6
- context_cond: bfloat16 [2048], P('sp'), may hold values from -6 to 6
- norm_gain: bfloat16 [2048], replicated, may hold values from 0.099609375 to 1.8984375
- mod_shift: bfloat16 [2048, 2048], P('sp', 'tp'), may hold values from -0.125 to 0.125
- mod_scale: bfloat16 [2048, 2048], P('sp', 'tp'), may hold values from -0.125 to 0.125
- mod_gate: bfloat16 [2048, 2048], P('sp', 'tp'), may hold values from -0.125 to 0.125
- w_query: bfloat16 [2048, 2048], P(None, 'tp'), may hold values from -0.125 to 0.125
- w_key: bfloat16 [2048, 2048], P(None, 'tp'), may hold values from -0.125 to 0.125
- w_value: bfloat16 [2048, 4096], P(None, 'tp'), may hold values from -0.125 to 0.125
- w_gate: bfloat16 [2048, 4096], P(None, 'tp'), may hold values from -0.125 to 0.125
- w_out: bfloat16 [4096, 2048], P('tp'), may hold values from -0.09375 to 0.09375
- decay_rate: float32 [2, 8], P(None, 'tp'), may hold values from 3.90625e-05 to 0.034
- context_gain: float32 [8], P('tp'), may hold values from 3 to 10
Outputs:
- mixed: bfloat16 [8192, 2048], P(('grp', 'sp', 'tp')), parts along dimension 0
The draws below stay inside these ranges and needn't reach their ends.
There are 2 independent parts, one for each index of `grp`. The reference program is written for one: setup_inputs(seed, part) draws one part's arguments, and reference() takes and returns one part's arrays. A program takes and returns all parts, laid end to end along the dimension named above; an argument that names none is the same for every part. Nothing has to cross between parts.
All inputs are finite; a program needn't handle non-finite values.
Results may differ from the reference program's by a relative error of at most 0.009.
Values may be sent and summed in bfloat16 or wider, within the bound.
A program may use at most 128 MiB of HBM per device.

```python
import math
import jax
import jax.numpy as jnp
from jax import lax

D = 2048
H = 8
DK = 256
DV = 512
GRID_W = 128
BLOCK = 128
NL = 4096
CTX = 1024
N_TP = 8


def draw_decay_rate(key, part):
    base = jax.random.fold_in(key, 17)
    pick_key, fast_key, slow_key = jax.random.split(base, 3)
    share = 0.5
    fast = jax.random.uniform(pick_key, (2, H), jnp.float32) < share
    fast_rate = jnp.exp(jax.random.uniform(fast_key, (2, H), jnp.float32, math.log(1.0 / 100.0), math.log(1.0 / 30.0)))
    slow_rate = jnp.exp(jax.random.uniform(slow_key, (2, H), jnp.float32, math.log(0.2), math.log(2.0))) / (NL + CTX)
    return jnp.where(fast, fast_rate, slow_rate).astype(jnp.float32)


def level_of(rng, extent, cuts, low, high):
    factor_of = 1.0
    for position, shards_of in cuts:
        heights = jax.random.uniform(jax.random.fold_in(jax.random.fold_in(rng, 6), position), (shards_of,), jnp.float32, low / len(cuts), high / len(cuts))
        factor_of = factor_of * jnp.repeat(jnp.exp(heights), extent[position] // shards_of).reshape((-1,) + (1,) * (len(extent) - 1 - position))
    return factor_of


def gaussian(key, shape, scale, reach, cuts=(), kind=jnp.bfloat16):
    entries = scale * jax.random.normal(key, shape, jnp.float32)
    if cuts:
        entries = entries * level_of(key, shape, cuts, -0.22, 0.18)
    return jnp.clip(entries, -reach, reach).astype(kind)


def setup_inputs(seed: int = 0, part: int = 0) -> dict:
    arg_keys = jax.random.split(jax.random.key(seed), 16)
    own_keys = jax.random.split(jax.random.fold_in(arg_keys[15], part), 16)
    latent = gaussian(own_keys[0], (NL, D), 1.0, 6.0, ((0, 128),))
    cond = gaussian(own_keys[1], (D,), 1.0, 6.0, ((0, 16),))
    context = gaussian(own_keys[2], (CTX, D), 1.0, 6.0, ((0, 16),))
    context_cond = gaussian(arg_keys[3], (D,), 1.0, 6.0, ((0, 16),))
    norm_gain = jnp.clip(1.0 + 0.18 * jax.random.normal(arg_keys[4], (D,), jnp.float32), 0.099609375, 1.8984375).astype(jnp.bfloat16)
    mod_shift = gaussian(arg_keys[5], (D, D), D ** -0.5, 0.125, ((0, 16), (1, 8)))
    mod_scale = gaussian(arg_keys[6], (D, D), D ** -0.5, 0.125, ((0, 16), (1, 8)))
    mod_gate = gaussian(arg_keys[7], (D, D), D ** -0.5, 0.125, ((0, 16), (1, 8)))
    w_query = gaussian(arg_keys[8], (D, H * DK), D ** -0.5, 0.125, ((1, 8),))
    w_key = gaussian(arg_keys[9], (D, H * DK), D ** -0.5, 0.125, ((1, 8),))
    w_value = gaussian(arg_keys[10], (D, H * DV), D ** -0.5, 0.125, ((1, 8),))
    w_gate = gaussian(arg_keys[11], (D, H * DV), D ** -0.5, 0.125, ((1, 8),))
    w_out = gaussian(arg_keys[12], (H * DV, D), (H * DV) ** -0.5, 0.09375, ((0, 8),))
    decay_rate = draw_decay_rate(jax.random.fold_in(arg_keys[15], 71), part)
    context_gain = jnp.clip(jnp.exp(math.log(10.0) - 1.2039728 * jax.random.uniform(arg_keys[14], (H,), jnp.float32) ** level_of(arg_keys[14], (H,), ((0, 8),), -0.2, 0.2)), 3.0, 10.0)
    return {"latent": latent, "cond": cond, "context": context, "context_cond": context_cond, "norm_gain": norm_gain, "mod_shift": mod_shift, "mod_scale": mod_scale, "mod_gate": mod_gate, "w_query": w_query, "w_key": w_key, "w_value": w_value, "w_gate": w_gate, "w_out": w_out, "decay_rate": decay_rate, "context_gain": context_gain}


norm_eps = 1e-06
rope_base = 10000.0
highest = lax.Precision.HIGHEST

def modulated(rows, norm_gain, shift, scale):
    values = rows.astype(jnp.float32)
    normed = values * lax.rsqrt(lax.optimization_barrier(jnp.mean(values * values, axis=-1, keepdims=True)) + norm_eps)
    return (normed * norm_gain.astype(jnp.float32) * (1.0 + scale) + shift).astype(jnp.bfloat16)

def rotate(vectors, positions):
    depth = vectors.shape[-1]
    freqs = depth // 4
    inv_freq = rope_base ** (-jnp.arange(freqs, dtype=jnp.float32) / freqs)
    grid_row = (positions // GRID_W).astype(jnp.float32)
    grid_col = (positions % GRID_W).astype(jnp.float32)
    angles = jnp.concatenate([grid_row[:, None] * inv_freq, grid_col[:, None] * inv_freq], axis=-1)[:, None, :]
    cos_table = jnp.cos(angles)
    sin_table = jnp.sin(angles)
    first_half, second_half = jnp.split(vectors, 2, axis=-1)
    return jnp.concatenate([first_half * cos_table - second_half * sin_table, second_half * cos_table + first_half * sin_table], axis=-1)

def rounded(values):
    return lax.optimization_barrier(values.astype(jnp.bfloat16)).astype(jnp.float32)

def context_states(ctx_key, ctx_value, fwd_rate, bwd_rate, context_gain):
    total = ctx_key.shape[0]
    place = jnp.arange(total, dtype=jnp.float32)[:, None]
    fwd_weight = jnp.exp(-fwd_rate[None, :] * (total - 1.0 - place))
    bwd_weight = jnp.exp(-bwd_rate[None, :] * place)
    keys_f = lax.optimization_barrier(ctx_key).astype(jnp.float32)
    values_f = lax.optimization_barrier(ctx_value).astype(jnp.float32)
    fwd_keys = rounded(keys_f * fwd_weight[:, :, None])
    bwd_keys = rounded(keys_f * bwd_weight[:, :, None])
    fwd_state = jnp.einsum('jhd,jhe->hde', fwd_keys, values_f, precision=highest)
    bwd_state = jnp.einsum('jhd,jhe->hde', bwd_keys, values_f, precision=highest)
    return (fwd_state * context_gain[:, None, None], bwd_state * context_gain[:, None, None])

def reference(latent, cond, context, context_cond, norm_gain, mod_shift, mod_scale, mod_gate, w_query, w_key, w_value, w_gate, w_out, decay_rate, context_gain):
    cond_rows = jax.nn.silu(jnp.stack([cond, context_cond]).astype(jnp.float32)).astype(jnp.bfloat16)
    shift = jnp.dot(cond_rows, mod_shift, preferred_element_type=jnp.float32)
    scale = jnp.dot(cond_rows, mod_scale, preferred_element_type=jnp.float32)
    gate = jnp.dot(cond_rows[0:1], mod_gate, preferred_element_type=jnp.float32)
    h_latent = modulated(latent, norm_gain, shift[0], scale[0])
    h_context = modulated(context, norm_gain, shift[1], scale[1])
    positions = jnp.arange(NL, dtype=jnp.int32)
    query = rotate(jnp.dot(h_latent, w_query, preferred_element_type=jnp.float32).reshape(NL, H, DK), positions).astype(jnp.bfloat16)
    keys = rotate(jnp.dot(h_latent, w_key, preferred_element_type=jnp.float32).reshape(NL, H, DK) * DK ** (-0.5), positions).astype(jnp.bfloat16)
    values = jnp.dot(h_latent, w_value, preferred_element_type=jnp.float32).astype(jnp.bfloat16).reshape(NL, H, DV)
    gate_pre = jnp.dot(h_latent, w_gate, preferred_element_type=jnp.float32).reshape(NL, H, DV)
    ctx_key = (jnp.dot(h_context, w_key, preferred_element_type=jnp.float32) * DK ** (-0.5)).astype(jnp.bfloat16)
    ctx_value = jnp.dot(h_context, w_value, preferred_element_type=jnp.float32).astype(jnp.bfloat16)
    fwd_rate = decay_rate[0]
    bwd_rate = decay_rate[1]
    ctx_fwd, ctx_bwd = context_states(ctx_key.reshape(CTX, H, DK), ctx_value.reshape(CTX, H, DV), fwd_rate, bwd_rate, context_gain)
    blocks = NL // BLOCK
    query_f = lax.optimization_barrier(query).astype(jnp.float32).reshape(blocks, BLOCK, H, DK)
    keys_f = lax.optimization_barrier(keys).astype(jnp.float32).reshape(blocks, BLOCK, H, DK)
    values_f = lax.optimization_barrier(values).astype(jnp.float32).reshape(blocks, BLOCK, H, DV)
    place = jnp.arange(BLOCK, dtype=jnp.float32)
    gap = place[:, None] - place[None, :]
    mask = jnp.where(gap >= 0, jnp.exp(-fwd_rate[:, None, None] * jnp.maximum(gap, 0.0)), 0.0) + jnp.where(gap <= 0, jnp.exp(-bwd_rate[:, None, None] * jnp.maximum(-gap, 0.0)), 0.0)
    scores = jnp.einsum('bihd,bjhd->bhij', query_f, keys_f, precision=highest)
    weights = lax.optimization_barrier((scores * mask[None]).astype(jnp.bfloat16)).astype(jnp.float32)
    retained = jnp.einsum('bhij,bjhe->bihe', weights, values_f, precision=highest)
    fwd_qw = jnp.exp(-fwd_rate[None, :] * (place[:, None] + 1.0))
    bwd_qw = jnp.exp(-bwd_rate[None, :] * (BLOCK - place[:, None]))
    fwd_kw = jnp.exp(-fwd_rate[None, :] * (BLOCK - 1.0 - place[:, None]))
    bwd_kw = jnp.exp(-bwd_rate[None, :] * place[:, None])
    fwd_keys = rounded(keys_f * fwd_kw[None, :, :, None])
    bwd_keys = rounded(keys_f * bwd_kw[None, :, :, None])
    fwd_step_decay = jnp.exp(-fwd_rate * BLOCK)[:, None, None]
    bwd_step_decay = jnp.exp(-bwd_rate * BLOCK)[:, None, None]

    def fwd_step(state, block):
        block_query, block_keys, block_values = block
        cross = jnp.einsum('ihd,hde->ihe', block_query, rounded(state), precision=highest) * fwd_qw[:, :, None]
        added = jnp.einsum('jhd,jhe->hde', block_keys, block_values, precision=highest)
        return (fwd_step_decay * state + added, cross)

    def bwd_step(state, block):
        block_query, block_keys, block_values = block
        cross = jnp.einsum('ihd,hde->ihe', block_query, rounded(state), precision=highest) * bwd_qw[:, :, None]
        added = jnp.einsum('jhd,jhe->hde', block_keys, block_values, precision=highest)
        return (bwd_step_decay * state + added, cross)
    fwd_final, fwd_cross = lax.scan(fwd_step, ctx_fwd, (query_f, fwd_keys, values_f))
    bwd_final, bwd_cross = lax.scan(bwd_step, ctx_bwd, (query_f, bwd_keys, values_f), reverse=True)
    retained = (retained + fwd_cross + bwd_cross).reshape(NL, H, DV)
    centre = lax.optimization_barrier(jnp.mean(retained, axis=-1, keepdims=True))
    variance = lax.optimization_barrier(jnp.mean(jnp.square(retained - centre), axis=-1, keepdims=True))
    normed = (retained - centre) * lax.rsqrt(variance + norm_eps)
    gated = (jax.nn.silu(gate_pre) * normed).astype(jnp.bfloat16).reshape(NL, H * DV)
    group_cols = H // N_TP * DV
    total = jnp.zeros((NL, D), jnp.float32)
    for group in range(N_TP):
        lower = group * group_cols
        partial_sum = jnp.dot(gated[:, lower:lower + group_cols], w_out[lower:lower + group_cols], preferred_element_type=jnp.float32).astype(jnp.bfloat16)
        total = total + lax.optimization_barrier(partial_sum).astype(jnp.float32)
    return (latent.astype(jnp.float32) + gate[0] * total).astype(jnp.bfloat16)
```

```python
import functools

import jax
import jax.numpy as jnp
import numpy as np
from jax import lax
from jax.experimental import pallas as pl
from jax.experimental.pallas import tpu as pltpu
from jax.sharding import PartitionSpec as P

GRID_W = 128
norm_eps = 1e-06
rope_base = 10000.0
MESH = pl.DeviceIdType.MESH
F32 = jnp.float32
BF16 = jnp.bfloat16
LANES = 128
CHUNK = 8
LEAD = 6


def rope_tables(rows, freqs):
    inv_freq = (rope_base ** (-np.arange(freqs, dtype=np.float32) / np.float32(freqs))).astype(np.float32)
    row_angles = np.arange(rows, dtype=np.float32)[:, None] * inv_freq
    col_angles = np.arange(GRID_W, dtype=np.float32)[:, None] * inv_freq
    row_angles = np.concatenate([row_angles, row_angles], axis=1).astype(np.float64)
    col_angles = np.concatenate([col_angles, col_angles], axis=1).astype(np.float64)
    return np.concatenate(
        [np.cos(row_angles), np.cos(col_angles), np.sin(row_angles), np.sin(col_angles)]
    ).astype(np.float32)


def silu(v):
    return v / (1.0 + jnp.exp(-v))


def dot(a, b):
    return jnp.dot(a, b, preferred_element_type=F32)


def dot_tokens(a, b):
    return lax.dot_general(a, b, (((0,), (0,)), ((), ())), preferred_element_type=F32)


def kernel(
    n_sp,
    n_tp,
    decay_ref,
    cgain_ref,
    latent_hbm,
    cond_hbm,
    context_hbm,
    gain_hbm,
    shift_hbm,
    scale_hbm,
    gate_hbm,
    wq_hbm,
    wk_hbm,
    wv_hbm,
    wg_hbm,
    wo_hbm,
    tab_hbm,
    out_ref,
    x_ref,
    c_ref,
    cond_ref,
    gain_ref,
    mshift_ref,
    mscale_ref,
    mgate_ref,
    wq_ref,
    wk_ref,
    wv_ref,
    wg_ref,
    wo_ref,
    tab_ref,
    part_ref,
    gpart_ref,
    precv_ref,
    grecv_ref,
    modf_ref,
    gatef_ref,
    r_ref,
    h_ref,
    k_ref,
    v_ref,
    lf_ref,
    lb_ref,
    cf_ref,
    cb_ref,
    ps_ref,
    pr_ref,
    ms_ref,
    mr_ref,
    q_ref,
    gp_ref,
    ret_ref,
    g_ref,
    osend_ref,
    orecv_ref,
    own_ref,
    xsend_ref,
    xrecv_ref,
    load_sem,
    msend_sem,
    mrecv_sem,
    gsend_sem,
    grecv_sem,
    tsend_sem,
    trecv_sem,
    hsend_sem,
    hrecv_sem,
    xsend_sem,
    xrecv_sem,
    pssem,
    prsem,
    mssem,
    mrsem,
    osend_sem,
    orecv_sem,
    rsend_sem,
    rrecv_sem,
):
    s = lax.axis_index("sp")
    t = lax.axis_index("tp")
    n_x = n_tp // 2
    x = t // 2
    c = t % 2
    partner = x * 2 + (1 - c)
    rows = x_ref.shape[1]
    D = x_ref.shape[2]
    span = rows * n_tp
    ctx_rows = c_ref.shape[0]
    dk = wk_ref.shape[1]
    dv = wv_ref.shape[1]
    n_chunks = dk // CHUNK

    def load(k, src, dst):
        copy = pltpu.make_async_copy(src, dst, load_sem.at[k])
        copy.start()
        return copy

    l_lat = load(0, latent_hbm, x_ref.at[t])
    l_cond = load(1, cond_hbm, cond_ref)
    l_ms = load(2, shift_hbm, mshift_ref)
    l_mc = load(3, scale_hbm, mscale_ref)
    l_mg = load(4, gate_hbm, mgate_ref)
    l_ctx = load(5, context_hbm, c_ref)
    l_gain = load(6, gain_hbm, gain_ref)
    l_tab = load(7, tab_hbm, tab_ref)
    l_wk = load(8, wk_hbm, wk_ref)
    l_wv = load(9, wv_hbm, wv_ref)
    l_wq = load(10, wq_hbm, wq_ref)
    l_wg = load(11, wg_hbm, wg_ref)
    l_wo = load(12, wo_hbm, wo_ref)

    barrier = pltpu.get_barrier_semaphore()
    for d in range(n_sp // 2, 0, -1):
        pl.semaphore_signal(barrier, inc=1, device_id={"sp": (s + d) % n_sp}, device_id_type=MESH)
        if 2 * d != n_sp:
            pl.semaphore_signal(barrier, inc=1, device_id={"sp": (s + n_sp - d) % n_sp}, device_id_type=MESH)
    for d in range(1, n_tp):
        pl.semaphore_signal(barrier, inc=1, device_id={"tp": (t + d) % n_tp}, device_id_type=MESH)

    l_cond.wait()
    crows = silu(cond_ref[...].astype(F32))
    rid = lax.broadcasted_iota(jnp.int32, (8, crows.shape[1]), 0)
    cl = jnp.broadcast_to(crows[0:1], rid.shape)
    cc = jnp.broadcast_to(crows[1:2], rid.shape)
    lhs_shift = jnp.where(rid == 0, cl, jnp.where(rid == 1, cc, 0.0)).astype(BF16)
    lhs_scale = jnp.where(rid == 2, cl, jnp.where(rid == 3, cc, 0.0)).astype(BF16)
    lhs_gate = jnp.where(rid == 0, cl, 0.0).astype(BF16)
    l_ms.wait()
    l_mc.wait()
    part = dot(lhs_shift, mshift_ref[...]) + dot(lhs_scale, mscale_ref[...])
    part_ref[...] = part[0:4]
    l_mg.wait()
    gpart_ref[...] = dot(lhs_gate, mgate_ref[...])[0:1]
    l_lat.wait()

    pl.semaphore_wait(barrier, n_sp - 1 + n_tp - 1)

    def sp_copy(d):
        return pltpu.make_async_remote_copy(
            src_ref=part_ref,
            dst_ref=precv_ref.at[d - 1],
            send_sem=msend_sem.at[d - 1],
            recv_sem=mrecv_sem.at[d - 1],
            device_id={"sp": (s + d) % n_sp},
            device_id_type=MESH,
        )

    def spg_copy(d):
        return pltpu.make_async_remote_copy(
            src_ref=gpart_ref,
            dst_ref=grecv_ref.at[d - 1],
            send_sem=gsend_sem.at[d - 1],
            recv_sem=grecv_sem.at[d - 1],
            device_id={"sp": (s + d) % n_sp},
            device_id_type=MESH,
        )

    order = [n_sp // 2]
    for d in range(n_sp // 2 - 1, 0, -1):
        order += [d, n_sp - d]
    for d in order:
        sp_copy(d).start()

    def lat_copy(block, to, sem):
        return pltpu.make_async_remote_copy(
            src_ref=x_ref.at[block],
            dst_ref=x_ref.at[block],
            send_sem=xsend_sem.at[sem],
            recv_sem=xrecv_sem.at[block],
            device_id={"tp": to},
            device_id_type=MESH,
        )

    hops = [1, n_x - 1] + list(range(2, n_x - 1))
    for d in hops:
        lat_copy(t, ((x + d) % n_x) * 2 + c, d).start()
    lat_copy(t, partner, 0).start()
    for d in order:
        spg_copy(d).start()

    l_ctx.wait()
    cv = c_ref[...].astype(F32)
    r = lax.rsqrt(jnp.mean(cv * cv, axis=-1, keepdims=True) + norm_eps)
    r_ref[pl.ds(span, ctx_rows), :] = jnp.broadcast_to(r, (ctx_rows, LANES))

    def forward(d):
        block = ((x + d) % n_x) * 2 + c
        lat_copy(block, block, d).wait_recv()
        lat_copy(block, partner, n_x + d).start()

    for d in hops[:2]:
        forward(d)

    total = part_ref[...]
    for d in range(1, n_sp):
        sp_copy(d).wait_recv()
        total = total + precv_ref[d - 1]
    modf_ref[t] = total

    def tp_copy(d, to_slot):
        return pltpu.make_async_remote_copy(
            src_ref=modf_ref.at[to_slot],
            dst_ref=modf_ref.at[to_slot],
            send_sem=tsend_sem.at[d - 1],
            recv_sem=trecv_sem.at[to_slot],
            device_id={"tp": (t + d) % n_tp},
            device_id_type=MESH,
        )

    for d in range(1, n_tp):
        tp_copy(d, t).start()

    for d in hops[2:]:
        forward(d)

    for d in range(1, n_x):
        other = ((x + d) % n_x) * 2 + (1 - c)
        lat_copy(other, other, 0).wait_recv()
    lat_copy(partner, partner, 0).wait_recv()

    for b in range(n_tp):
        xv = x_ref[b].astype(F32)
        r = lax.rsqrt(jnp.mean(xv * xv, axis=-1, keepdims=True) + norm_eps)
        r_ref[pl.ds(b * rows, rows), :] = jnp.broadcast_to(r, (rows, LANES))

    neg_a = -decay_ref[0, 0]
    neg_b = -decay_ref[1, 0]
    cgain = cgain_ref[0]

    l_tab.wait()
    n_rows_total = tab_ref.shape[0] // 2 - GRID_W
    half = tab_ref.shape[1] // 2
    left = lax.broadcasted_iota(jnp.int32, (GRID_W, tab_ref.shape[1]), 1) < half

    def table(base):
        pieces = []
        for b in range(span // GRID_W):
            row = tab_ref[pl.ds(base + s * (span // GRID_W) + b, 1), :]
            col = tab_ref[pl.ds(base + n_rows_total, GRID_W), :]
            pieces.append(jnp.where(left, jnp.broadcast_to(row, col.shape), col))
        return jnp.concatenate(pieces, axis=0)

    cos_t = table(0)
    sin_t = table(n_rows_total + GRID_W)

    def rotate(v):
        u, w = v[:, : dk // 2], v[:, dk // 2 :]
        return jnp.concatenate([u * cos_t - w * sin_t, w * cos_t + u * sin_t], axis=1)

    l_gain.wait()
    l_wk.wait()
    l_wv.wait()
    for d in range(1, n_tp):
        tp_copy(n_tp - d, (t + d) % n_tp).wait_recv()

    cols_per = D // n_tp
    for k in range(D // LANES):
        cols = pl.ds(k * LANES, LANES)
        owner, off = divmod(k * LANES, cols_per)
        m = modf_ref[owner, :, pl.ds(off, LANES)]
        g = gain_ref[:, cols].astype(F32)
        f_lat = g * (1.0 + m[2:3])
        f_ctx = g * (1.0 + m[3:4])
        xv = x_ref[:, :, cols].reshape(span, LANES).astype(F32)
        h_ref[pl.ds(0, span), cols] = (xv * r_ref[pl.ds(0, span), :] * f_lat + m[0:1]).astype(BF16)
        cv = c_ref[:, cols].astype(F32)
        h_ref[pl.ds(span, ctx_rows), cols] = (cv * r_ref[pl.ds(span, ctx_rows), :] * f_ctx + m[1:2]).astype(BF16)

    kk = dot(h_ref[...], wk_ref[...]) * dk ** (-0.5)
    keys = rotate(kk[:span])
    k_ref[...] = keys.astype(BF16)
    keys = k_ref[...].astype(F32)
    ctx_key = kk[span:].astype(BF16).astype(F32)
    vv = dot(h_ref[...], wv_ref[...]).astype(BF16)
    v_ref[...] = vv[:span]
    values = vv[:span]
    ctx_val = vv[span:]

    place = lax.broadcasted_iota(jnp.int32, (span, 1), 0).astype(F32)
    fwd_keys = (keys * jnp.exp(neg_a * (span - 1.0 - place))).astype(BF16)
    bwd_keys = (keys * jnp.exp(neg_b * place)).astype(BF16)
    cplace = (lax.broadcasted_iota(jnp.int32, (ctx_rows, 1), 0) + s * ctx_rows).astype(F32)
    ctx_total = ctx_rows * n_sp
    cf_keys = (ctx_key * jnp.exp(neg_a * (ctx_total - 1.0 - cplace))).astype(BF16)
    cb_keys = (ctx_key * jnp.exp(neg_b * cplace)).astype(BF16)

    def scalar_exp(v):
        return jnp.exp(jnp.full((1, LANES), v, F32))[:, 0:1]

    sf = s.astype(F32)
    cf = cgain * dot_tokens(cf_keys, ctx_val)
    cf_ref[...] = cf
    lf_ref[...] = dot_tokens(fwd_keys, values) + scalar_exp(neg_a * (span * (sf + 1.0))) * cf
    cb = cgain * dot_tokens(cb_keys, ctx_val)
    cb_ref[...] = cb
    lb_ref[...] = dot_tokens(bwd_keys, values) + scalar_exp(neg_b * (span * (n_sp - sf))) * cb

    a_step = scalar_exp(neg_a * float(span))
    b_step = scalar_exp(neg_b * float(span))

    @pl.when(s == 0)
    def _():
        pr_ref[...] = jnp.zeros_like(pr_ref)

    @pl.when(s == n_sp - 1)
    def _():
        mr_ref[...] = jnp.zeros_like(mr_ref)

    def up_copy(j):
        return pltpu.make_async_remote_copy(
            src_ref=ps_ref.at[j],
            dst_ref=pr_ref.at[j],
            send_sem=pssem.at[j],
            recv_sem=prsem.at[j],
            device_id={"sp": (s + 1) % n_sp},
            device_id_type=MESH,
        )

    def down_copy(j):
        return pltpu.make_async_remote_copy(
            src_ref=ms_ref.at[j],
            dst_ref=mr_ref.at[j],
            send_sem=mssem.at[j],
            recv_sem=mrsem.at[j],
            device_id={"sp": (s + n_sp - 1) % n_sp},
            device_id_type=MESH,
        )

    def local_part():
        l_wq.wait()
        h = h_ref[pl.ds(0, span), :]
        query = rotate(dot(h, wq_ref[...])).astype(BF16)
        q_ref[...] = query
        scores = lax.dot_general(query, k_ref[...], (((1,), (1,)), ((), ())), preferred_element_type=F32)
        gap = (
            lax.broadcasted_iota(jnp.int32, (span, span), 0) - lax.broadcasted_iota(jnp.int32, (span, span), 1)
        ).astype(F32)
        mask = jnp.where(gap >= 0, jnp.exp(neg_a * jnp.maximum(gap, 0.0)), 0.0) + jnp.where(
            gap <= 0, jnp.exp(neg_b * jnp.maximum(-gap, 0.0)), 0.0
        )
        ret_ref[...] = dot((scores * mask).astype(BF16), v_ref[...])
        l_wg.wait()
        gp_ref[...] = silu(dot(h, wg_ref[...]))

    gap_s = n_sp - 1 - 2 * s
    early = s < n_sp // 2
    lag = jnp.minimum(jnp.where(early, gap_s, -gap_s) * LEAD, n_chunks)
    lag_up = jnp.where(early, 0, lag)
    lag_down = jnp.where(early, lag, 0)
    near_end = jnp.minimum(s, n_sp - 1 - s) < 4
    when_local = jnp.where(near_end, n_chunks, 0)

    def step(i, carry):
        @pl.when(i == when_local)
        def _():
            local_part()

        j_up = i - lag_up

        @pl.when((j_up >= 0) & (j_up < n_chunks))
        def _():
            j = j_up

            @pl.when(s > 0)
            def _():
                up_copy(j).wait_recv()

            @pl.when(s < n_sp - 1)
            def _():
                sl = pl.ds(pl.multiple_of(j * CHUNK, CHUNK), CHUNK)
                ps_ref[j, 0] = (a_step * pr_ref[j, 0].astype(F32) + lf_ref[sl, :]).astype(BF16)
                ps_ref[j, 1] = (pr_ref[j, 1].astype(F32) + cb_ref[sl, :]).astype(BF16)
                up_copy(j).start()

        j_dn = i - lag_down

        @pl.when((j_dn >= 0) & (j_dn < n_chunks))
        def _():
            j = j_dn

            @pl.when(s < n_sp - 1)
            def _():
                down_copy(j).wait_recv()

            @pl.when(s > 0)
            def _():
                sl = pl.ds(pl.multiple_of(j * CHUNK, CHUNK), CHUNK)
                ms_ref[j, 0] = (b_step * mr_ref[j, 0].astype(F32) + lb_ref[sl, :]).astype(BF16)
                ms_ref[j, 1] = (mr_ref[j, 1].astype(F32) + cf_ref[sl, :]).astype(BF16)
                down_copy(j).start()

        return carry

    lax.fori_loop(0, 2 * n_chunks, step, 0)

    ca = scalar_exp(neg_a * (span * sf))
    cbk = scalar_exp(neg_b * (span * (n_sp - 1.0 - sf)))
    up_in = pr_ref[...]
    down_in = mr_ref[...]
    s_fwd = up_in[:, 0].reshape(dk, dv).astype(F32) + ca * (
        down_in[:, 1].reshape(dk, dv).astype(F32) + cf_ref[...]
    )
    s_bwd = down_in[:, 0].reshape(dk, dv).astype(F32) + cbk * (
        up_in[:, 1].reshape(dk, dv).astype(F32) + cb_ref[...]
    )
    query = q_ref[...]
    ret = (
        ret_ref[...]
        + dot(query, s_fwd.astype(BF16)) * jnp.exp(neg_a * (place + 1.0))
        + dot(query, s_bwd.astype(BF16)) * jnp.exp(neg_b * (span - place))
    )
    centre = jnp.mean(ret, axis=-1, keepdims=True)
    ret = ret - centre
    variance = jnp.mean(ret * ret, axis=-1, keepdims=True)
    gated = (gp_ref[...] * (ret * lax.rsqrt(variance + norm_eps))).astype(BF16)
    g_ref[...] = gated.reshape(n_tp, rows, dv)

    l_wo.wait()

    def rows_of(core):
        return jnp.concatenate([g_ref[2 * k + core] for k in range(n_x)], axis=0)

    def pair_copy():
        return pltpu.make_async_remote_copy(
            src_ref=osend_ref,
            dst_ref=orecv_ref,
            send_sem=osend_sem,
            recv_sem=orecv_sem,
            device_id={"tp": partner},
            device_id_type=MESH,
        )

    osend_ref[...] = dot(rows_of(1 - c), wo_ref[...]).astype(BF16).reshape(n_x, rows, D)
    pair_copy().start()
    own_ref[...] = dot(rows_of(c), wo_ref[...]).reshape(n_x, rows, D)
    pair_copy().wait_recv()

    def out_copy(d):
        return pltpu.make_async_remote_copy(
            src_ref=xsend_ref.at[d - 1],
            dst_ref=xrecv_ref.at[d - 1],
            send_sem=rsend_sem.at[d - 1],
            recv_sem=rrecv_sem.at[d - 1],
            device_id={"tp": ((x + d) % n_x) * 2 + c},
            device_id_type=MESH,
        )

    for d in hops:
        to = (x + d) % n_x
        xsend_ref[d - 1] = (own_ref[to] + orecv_ref[to].astype(F32)).astype(BF16)
        out_copy(d).start()
    acc = own_ref[x] + orecv_ref[x].astype(F32)

    gtotal = gpart_ref[...]
    for d in range(1, n_sp):
        spg_copy(d).wait_recv()
        gtotal = gtotal + grecv_ref[d - 1]
    gatef_ref[t] = gtotal

    def tpg_copy(d, slot):
        return pltpu.make_async_remote_copy(
            src_ref=gatef_ref.at[slot],
            dst_ref=gatef_ref.at[slot],
            send_sem=hsend_sem.at[d - 1],
            recv_sem=hrecv_sem.at[slot],
            device_id={"tp": (t + d) % n_tp},
            device_id_type=MESH,
        )

    for d in range(1, n_tp):
        tpg_copy(d, t).start()
    for d in range(1, n_tp):
        tpg_copy(n_tp - d, (t + d) % n_tp).wait_recv()
    gate = jnp.concatenate([gatef_ref[k] for k in range(n_tp)], axis=1)

    for d in hops:
        out_copy(d).wait_recv()
        acc = acc + xrecv_ref[d - 1].astype(F32)
    out_ref[...] = (x_ref[t].astype(F32) + gate * acc).astype(BF16)

    for d in range(1, n_sp):
        sp_copy(d).wait_send()
        spg_copy(d).wait_send()
    for d in range(1, n_tp):
        tp_copy(d, t).wait_send()
        tpg_copy(d, t).wait_send()
    lat_copy(t, partner, 0).wait_send()
    for d in range(1, n_x):
        lat_copy(t, partner, d).wait_send()
        lat_copy(t, partner, n_x + d).wait_send()
        out_copy(d).wait_send()
    pair_copy().wait_send()

    @pl.when(s < n_sp - 1)
    def _():
        @pl.loop(0, n_chunks)
        def _(j):
            up_copy(j).wait_send()

    @pl.when(s > 0)
    def _():
        @pl.loop(0, n_chunks)
        def _(j):
            down_copy(j).wait_send()


def body(
    n_sp,
    n_tp,
    latent,
    cond,
    context,
    context_cond,
    norm_gain,
    mod_shift,
    mod_scale,
    mod_gate,
    w_query,
    w_key,
    w_value,
    w_gate,
    w_out,
    decay_rate,
    context_gain,
):
    rows, D = latent.shape
    span = rows * n_tp
    ctx_rows = context.shape[0]
    dk, dv = w_key.shape[1], w_value.shape[1]
    cols = D // n_tp
    n_x = n_tp // 2
    n_chunks = dk // CHUNK
    tab = jnp.asarray(rope_tables(span * n_sp // GRID_W, dk // 4))
    any_spec = pl.BlockSpec(memory_space=pl.ANY)
    smem = pl.BlockSpec(memory_space=pltpu.SMEM)
    dma = pltpu.SemaphoreType.DMA
    vm = pltpu.VMEM
    scratch = [
        vm((n_tp, rows, D), BF16),
        vm((ctx_rows, D), BF16),
        vm((2, cond.shape[0]), BF16),
        vm((1, D), BF16),
        vm(mod_shift.shape, BF16),
        vm(mod_scale.shape, BF16),
        vm(mod_gate.shape, BF16),
        vm(w_query.shape, BF16),
        vm(w_key.shape, BF16),
        vm(w_value.shape, BF16),
        vm(w_gate.shape, BF16),
        vm(w_out.shape, BF16),
        vm(tab.shape, F32),
        vm((4, cols), F32),
        vm((1, cols), F32),
        vm((n_sp - 1, 4, cols), F32),
        vm((n_sp - 1, 1, cols), F32),
        vm((n_tp, 4, cols), F32),
        vm((n_tp, 1, cols), F32),
        vm((span + ctx_rows, LANES), F32),
        vm((span + ctx_rows, D), BF16),
        vm((span, dk), BF16),
        vm((span, dv), BF16),
        vm((dk, dv), F32),
        vm((dk, dv), F32),
        vm((dk, dv), F32),
        vm((dk, dv), F32),
        vm((n_chunks, 2, CHUNK, dv), BF16),
        vm((n_chunks, 2, CHUNK, dv), BF16),
        vm((n_chunks, 2, CHUNK, dv), BF16),
        vm((n_chunks, 2, CHUNK, dv), BF16),
        vm((span, dk), BF16),
        vm((span, dv), F32),
        vm((span, dv), F32),
        vm((n_tp, rows, dv), BF16),
        vm((n_x, rows, D), BF16),
        vm((n_x, rows, D), BF16),
        vm((n_x, rows, D), F32),
        vm((n_x - 1, rows, D), BF16),
        vm((n_x - 1, rows, D), BF16),
        dma((13,)),
        dma((n_sp - 1,)),
        dma((n_sp - 1,)),
        dma((n_sp - 1,)),
        dma((n_sp - 1,)),
        dma((n_tp - 1,)),
        dma((n_tp,)),
        dma((n_tp - 1,)),
        dma((n_tp,)),
        dma((2 * n_x,)),
        dma((n_tp,)),
        dma((n_chunks,)),
        dma((n_chunks,)),
        dma((n_chunks,)),
        dma((n_chunks,)),
        dma,
        dma,
        dma((n_x - 1,)),
        dma((n_x - 1,)),
    ]
    return pl.pallas_call(
        functools.partial(kernel, n_sp, n_tp),
        out_shape=jax.ShapeDtypeStruct(latent.shape, BF16),
        in_specs=[smem, smem] + [any_spec] * 13,
        out_specs=pl.BlockSpec(memory_space=pltpu.VMEM),
        scratch_shapes=scratch,
        compiler_params=pltpu.CompilerParams(
            collective_id=0, has_side_effects=True, vmem_limit_bytes=60 * 1024 * 1024
        ),
        name="layer",
    )(
        decay_rate,
        context_gain,
        latent,
        jnp.stack([cond, context_cond]),
        context,
        norm_gain.reshape(1, D),
        mod_shift,
        mod_scale,
        mod_gate,
        w_query,
        w_key,
        w_value,
        w_gate,
        w_out,
        tab,
    )


def solution(mesh):
    return jax.shard_map(
        functools.partial(body, mesh.shape["sp"], mesh.shape["tp"]),
        mesh=mesh,
        in_specs=(
            P(("grp", "sp", "tp"), None),
            P(("grp", "sp")),
            P(("grp", "sp"), None),
            P("sp"),
            P(),
            P("sp", "tp"),
            P("sp", "tp"),
            P("sp", "tp"),
            P(None, "tp"),
            P(None, "tp"),
            P(None, "tp"),
            P(None, "tp"),
            P("tp", None),
            P(None, "tp"),
            P("tp"),
        ),
        out_specs=P(("grp", "sp", "tp"), None),
        check_vma=False,
    )
```

```python
import functools

import jax
import jax.numpy as jnp
import numpy as np
from jax import lax
from jax.experimental import pallas as pl
from jax.experimental.pallas import tpu as pltpu
from jax.sharding import PartitionSpec as P

GRID_W = 128
norm_eps = 1e-06
rope_base = 10000.0
MESH = pl.DeviceIdType.MESH
F32 = jnp.float32
BF16 = jnp.bfloat16
LANES = 128
CHUNK = 8
LEAD = 6


def rope_tables(rows, freqs):
    inv_freq = (rope_base ** (-np.arange(freqs, dtype=np.float32) / np.float32(freqs))).astype(np.float32)
    row_angles = np.arange(rows, dtype=np.float32)[:, None] * inv_freq
    col_angles = np.arange(GRID_W, dtype=np.float32)[:, None] * inv_freq
    row_angles = np.concatenate([row_angles, row_angles], axis=1).astype(np.float64)
    col_angles = np.concatenate([col_angles, col_angles], axis=1).astype(np.float64)
    return np.concatenate(
        [np.cos(row_angles), np.cos(col_angles), np.sin(row_angles), np.sin(col_angles)]
    ).astype(np.float32)


def silu(v):
    return v / (1.0 + jnp.exp(-v))


def dot(a, b):
    return jnp.dot(a, b, preferred_element_type=F32)


def dot_tokens(a, b):
    return lax.dot_general(a, b, (((0,), (0,)), ((), ())), preferred_element_type=F32)


def kernel(
    n_sp,
    n_tp,
    decay_ref,
    cgain_ref,
    latent_hbm,
    cond_hbm,
    ccond_hbm,
    context_hbm,
    gain_hbm,
    shift_hbm,
    scale_hbm,
    gate_hbm,
    wq_hbm,
    wk_hbm,
    wv_hbm,
    wg_hbm,
    wo_hbm,
    tab_hbm,
    out_ref,
    x_ref,
    c_ref,
    cond_ref,
    ccond_ref,
    gain_ref,
    mshift_ref,
    mscale_ref,
    mgate_ref,
    wq_ref,
    wk_ref,
    wv_ref,
    wg_ref,
    wo_ref,
    tab_ref,
    part_ref,
    gpart_ref,
    precv_ref,
    grecv_ref,
    modf_ref,
    gatef_ref,
    r_ref,
    h_ref,
    k_ref,
    v_ref,
    lf_ref,
    lb_ref,
    cf_ref,
    cb_ref,
    us_ref,
    ur_ref,
    ds_ref,
    dr_ref,
    bs_ref,
    br_ref,
    cs_ref,
    cr_ref,
    fin_ref,
    q_ref,
    gp_ref,
    ret_ref,
    g_ref,
    osend_ref,
    orecv_ref,
    own_ref,
    xsend_ref,
    xrecv_ref,
    load_sem,
    msend_sem,
    mrecv_sem,
    gsend_sem,
    grecv_sem,
    tsend_sem,
    trecv_sem,
    hsend_sem,
    hrecv_sem,
    xsend_sem,
    xrecv_sem,
    ussem,
    ursem,
    dssem,
    drsem,
    bssem,
    brsem,
    cssem,
    crsem,
    osend_sem,
    orecv_sem,
    rsend_sem,
    rrecv_sem,
):
    s = lax.axis_index("sp")
    t = lax.axis_index("tp")
    n_x = n_tp // 2
    x = t // 2
    c = t % 2
    partner = x * 2 + (1 - c)
    rows = x_ref.shape[1]
    D = x_ref.shape[2]
    span = rows * n_tp
    ctx_rows = c_ref.shape[0]
    dk = wk_ref.shape[1]
    dv = wv_ref.shape[1]
    n_chunks = dk // CHUNK

    def load(k, src, dst):
        copy = pltpu.make_async_copy(src, dst, load_sem.at[k])
        copy.start()
        return copy

    l_lat = load(0, latent_hbm, x_ref.at[t])
    l_cond = load(1, cond_hbm, cond_ref)
    l_ccond = load(13, ccond_hbm, ccond_ref)
    l_ms = load(2, shift_hbm, mshift_ref)
    l_mc = load(3, scale_hbm, mscale_ref)
    l_mg = load(4, gate_hbm, mgate_ref)
    l_ctx = load(5, context_hbm, c_ref)
    l_gain = load(6, gain_hbm, gain_ref)
    l_tab = load(7, tab_hbm, tab_ref)
    l_wk = load(8, wk_hbm, wk_ref)
    l_wv = load(9, wv_hbm, wv_ref)
    l_wq = load(10, wq_hbm, wq_ref)
    l_wg = load(11, wg_hbm, wg_ref)
    l_wo = load(12, wo_hbm, wo_ref)

    barrier = pltpu.get_barrier_semaphore()
    for d in range(n_sp // 2, 0, -1):
        pl.semaphore_signal(barrier, inc=1, device_id={"sp": (s + d) % n_sp}, device_id_type=MESH)
        if 2 * d != n_sp:
            pl.semaphore_signal(barrier, inc=1, device_id={"sp": (s + n_sp - d) % n_sp}, device_id_type=MESH)
    for d in range(1, n_tp):
        pl.semaphore_signal(barrier, inc=1, device_id={"tp": (t + d) % n_tp}, device_id_type=MESH)

    l_cond.wait()
    l_ccond.wait()
    rid = lax.broadcasted_iota(jnp.int32, (8, cond_ref.shape[1]), 0)
    cl = jnp.broadcast_to(silu(cond_ref[...].astype(F32)), rid.shape)
    cc = jnp.broadcast_to(silu(ccond_ref[...].astype(F32)), rid.shape)
    lhs_shift = jnp.where(rid == 0, cl, jnp.where(rid == 1, cc, 0.0)).astype(BF16)
    lhs_scale = jnp.where(rid == 2, cl, jnp.where(rid == 3, cc, 0.0)).astype(BF16)
    lhs_gate = jnp.where(rid == 0, cl, 0.0).astype(BF16)
    l_ms.wait()
    l_mc.wait()
    part = dot(lhs_shift, mshift_ref[...]) + dot(lhs_scale, mscale_ref[...])
    part_ref[...] = part[0:4]
    l_mg.wait()
    gpart_ref[...] = dot(lhs_gate, mgate_ref[...])[0:1]
    l_lat.wait()

    pl.semaphore_wait(barrier, n_sp - 1 + n_tp - 1)

    def sp_copy(d):
        return pltpu.make_async_remote_copy(
            src_ref=part_ref,
            dst_ref=precv_ref.at[d - 1],
            send_sem=msend_sem.at[d - 1],
            recv_sem=mrecv_sem.at[d - 1],
            device_id={"sp": (s + d) % n_sp},
            device_id_type=MESH,
        )

    def spg_copy(d):
        return pltpu.make_async_remote_copy(
            src_ref=gpart_ref,
            dst_ref=grecv_ref.at[d - 1],
            send_sem=gsend_sem.at[d - 1],
            recv_sem=grecv_sem.at[d - 1],
            device_id={"sp": (s + d) % n_sp},
            device_id_type=MESH,
        )

    order = [n_sp // 2]
    for d in range(n_sp // 2 - 1, 0, -1):
        order += [d, n_sp - d]
    for d in order:
        sp_copy(d).start()

    def lat_copy(block, to, sem):
        return pltpu.make_async_remote_copy(
            src_ref=x_ref.at[block],
            dst_ref=x_ref.at[block],
            send_sem=xsend_sem.at[sem],
            recv_sem=xrecv_sem.at[block],
            device_id={"tp": to},
            device_id_type=MESH,
        )

    hops = [1, n_x - 1] + list(range(2, n_x - 1))
    for d in hops:
        lat_copy(t, ((x + d) % n_x) * 2 + c, d).start()
    lat_copy(t, partner, 0).start()
    for d in order:
        spg_copy(d).start()

    l_ctx.wait()
    cv = c_ref[...].astype(F32)
    r = lax.rsqrt(jnp.mean(cv * cv, axis=-1, keepdims=True) + norm_eps)
    r_ref[pl.ds(span, ctx_rows), :] = jnp.broadcast_to(r, (ctx_rows, LANES))

    def forward(d):
        block = ((x + d) % n_x) * 2 + c
        lat_copy(block, block, d).wait_recv()
        lat_copy(block, partner, n_x + d).start()

    for d in hops[:2]:
        forward(d)

    total = part_ref[...]
    for d in range(1, n_sp):
        sp_copy(d).wait_recv()
        total = total + precv_ref[d - 1]
    modf_ref[t] = total

    def tp_copy(d, to_slot):
        return pltpu.make_async_remote_copy(
            src_ref=modf_ref.at[to_slot],
            dst_ref=modf_ref.at[to_slot],
            send_sem=tsend_sem.at[d - 1],
            recv_sem=trecv_sem.at[to_slot],
            device_id={"tp": (t + d) % n_tp},
            device_id_type=MESH,
        )

    for d in range(1, n_tp):
        tp_copy(d, t).start()

    for d in hops[2:]:
        forward(d)

    for d in range(1, n_x):
        other = ((x + d) % n_x) * 2 + (1 - c)
        lat_copy(other, other, 0).wait_recv()
    lat_copy(partner, partner, 0).wait_recv()

    for b in range(n_tp):
        xv = x_ref[b].astype(F32)
        r = lax.rsqrt(jnp.mean(xv * xv, axis=-1, keepdims=True) + norm_eps)
        r_ref[pl.ds(b * rows, rows), :] = jnp.broadcast_to(r, (rows, LANES))

    neg_a = -decay_ref[0]
    neg_b = -decay_ref[1]
    cgain = cgain_ref[0]

    l_tab.wait()
    n_rows_total = tab_ref.shape[0] // 2 - GRID_W
    half = tab_ref.shape[1] // 2
    left = lax.broadcasted_iota(jnp.int32, (GRID_W, tab_ref.shape[1]), 1) < half

    def table(base):
        pieces = []
        for b in range(span // GRID_W):
            row = tab_ref[pl.ds(base + s * (span // GRID_W) + b, 1), :]
            col = tab_ref[pl.ds(base + n_rows_total, GRID_W), :]
            pieces.append(jnp.where(left, jnp.broadcast_to(row, col.shape), col))
        return jnp.concatenate(pieces, axis=0)

    cos_t = table(0)
    sin_t = table(n_rows_total + GRID_W)

    def rotate(v):
        u, w = v[:, : dk // 2], v[:, dk // 2 :]
        return jnp.concatenate([u * cos_t - w * sin_t, w * cos_t + u * sin_t], axis=1)

    l_gain.wait()
    l_wk.wait()
    l_wv.wait()
    for d in range(1, n_tp):
        tp_copy(n_tp - d, (t + d) % n_tp).wait_recv()

    cols_per = D // n_tp
    for k in range(D // LANES):
        cols = pl.ds(k * LANES, LANES)
        owner, off = divmod(k * LANES, cols_per)
        m = modf_ref[owner, :, pl.ds(off, LANES)]
        g = gain_ref[k : k + 1, :].astype(F32)
        f_lat = g * (1.0 + m[2:3])
        f_ctx = g * (1.0 + m[3:4])
        xv = x_ref[:, :, cols].reshape(span, LANES).astype(F32)
        h_ref[pl.ds(0, span), cols] = (xv * r_ref[pl.ds(0, span), :] * f_lat + m[0:1]).astype(BF16)
        cv = c_ref[:, cols].astype(F32)
        h_ref[pl.ds(span, ctx_rows), cols] = (cv * r_ref[pl.ds(span, ctx_rows), :] * f_ctx + m[1:2]).astype(BF16)

    kk = dot(h_ref[...], wk_ref[...]) * dk ** (-0.5)
    keys = rotate(kk[:span])
    k_ref[...] = keys.astype(BF16)
    keys = k_ref[...].astype(F32)
    ctx_key = kk[span:].astype(BF16).astype(F32)
    vv = dot(h_ref[...], wv_ref[...]).astype(BF16)
    v_ref[...] = vv[:span]
    values = vv[:span]
    ctx_val = vv[span:]

    place = lax.broadcasted_iota(jnp.int32, (span, 1), 0).astype(F32)
    fwd_keys = (keys * jnp.exp(neg_a * (span - 1.0 - place))).astype(BF16)
    bwd_keys = (keys * jnp.exp(neg_b * place)).astype(BF16)
    cplace = (lax.broadcasted_iota(jnp.int32, (ctx_rows, 1), 0) + s * ctx_rows).astype(F32)
    ctx_total = ctx_rows * n_sp
    cf_keys = (ctx_key * jnp.exp(neg_a * (ctx_total - 1.0 - cplace))).astype(BF16)
    cb_keys = (ctx_key * jnp.exp(neg_b * cplace)).astype(BF16)

    def scalar_exp(v):
        return jnp.exp(jnp.full((1, LANES), v, F32))[:, 0:1]

    sf = s.astype(F32)
    cf = cgain * dot_tokens(cf_keys, ctx_val)
    cf_ref[...] = cf
    lf_ref[...] = dot_tokens(fwd_keys, values) + scalar_exp(neg_a * (span * (sf + 1.0))) * cf
    cb = cgain * dot_tokens(cb_keys, ctx_val)
    cb_ref[...] = cb
    lb_ref[...] = dot_tokens(bwd_keys, values) + scalar_exp(neg_b * (span * (n_sp - sf))) * cb

    a_step = scalar_exp(neg_a * float(span))
    b_step = scalar_exp(neg_b * float(span))

    top, mid, low = n_sp - 1, n_sp // 2, n_sp // 4

    def chain(send, recv, ssem, rsem, to):
        def copy(j, src=None):
            return pltpu.make_async_remote_copy(
                src_ref=(send if src is None else src).at[j],
                dst_ref=recv.at[j],
                send_sem=ssem,
                recv_sem=rsem.at[j],
                device_id={"sp": to},
                device_id_type=MESH,
            )

        return copy

    above, under = (s + 1) % n_sp, (s + n_sp - 1) % n_sp
    up_copy = chain(us_ref, ur_ref, ussem, ursem, above)
    down_copy = chain(ds_ref, dr_ref, dssem, drsem, under)
    below_copy = chain(bs_ref, br_ref, bssem, brsem, under)
    carry_copy = chain(cs_ref, cr_ref, cssem, crsem, above)
    up_recv, up_send = s > 0, s < top
    down_recv, down_send = (s >= low) & (s < top), s > low
    below_recv, below_send = s < mid - 1, (s > 0) & (s < mid)
    carry_recv, carry_send = (s > mid) | (s < low), s >= mid
    carry_pass = s < low - 1

    for first, ref in ((0, ur_ref), (top, dr_ref), (mid - 1, br_ref), (mid, cr_ref)):

        @pl.when(s == first)
        def _(ref=ref):
            ref[...] = jnp.zeros_like(ref)

    carry_w = scalar_exp(neg_b * (span * jnp.maximum(sf - mid, 0.0)))

    gtotal = gpart_ref[...]
    for d in range(1, n_sp):
        spg_copy(d).wait_recv()
        gtotal = gtotal + grecv_ref[d - 1]
    gatef_ref[t] = gtotal

    def tpg_copy(d, slot):
        return pltpu.make_async_remote_copy(
            src_ref=gatef_ref.at[slot],
            dst_ref=gatef_ref.at[slot],
            send_sem=hsend_sem.at[d - 1],
            recv_sem=hrecv_sem.at[slot],
            device_id={"tp": (t + d) % n_tp},
            device_id_type=MESH,
        )

    for d in range(1, n_tp):
        tpg_copy(d, t).start()

    def local_part():
        l_wq.wait()
        h = h_ref[pl.ds(0, span), :]
        query = rotate(dot(h, wq_ref[...])).astype(BF16)
        q_ref[...] = query
        scores = lax.dot_general(query, k_ref[...], (((1,), (1,)), ((), ())), preferred_element_type=F32)
        gap = (
            lax.broadcasted_iota(jnp.int32, (span, span), 0) - lax.broadcasted_iota(jnp.int32, (span, span), 1)
        ).astype(F32)
        mask = jnp.where(gap >= 0, jnp.exp(neg_a * jnp.maximum(gap, 0.0)), 0.0) + jnp.where(
            gap <= 0, jnp.exp(neg_b * jnp.maximum(-gap, 0.0)), 0.0
        )
        ret_ref[...] = dot((scores * mask).astype(BF16), v_ref[...])
        l_wg.wait()
        gp_ref[...] = silu(dot(h, wg_ref[...]))

    late = 4 * n_sp
    at_up = s
    at_down = jnp.where(s >= low, top - s, late)
    at_below = jnp.where(s < mid, mid - 1 - s, late)
    at_carry = jnp.where(s >= mid, s - mid, jnp.where(s < low, s + n_sp - mid, late))
    first = jnp.minimum(jnp.minimum(at_up, at_down), jnp.minimum(at_below, at_carry))
    lag_up = (at_up - first) * LEAD
    lag_down = (at_down - first) * LEAD
    lag_below = (at_below - first) * LEAD
    lag_carry = (at_carry - first) * LEAD
    n_steps = n_chunks + n_sp * LEAD

    when_local = 0
    for k in range(n_sp):
        if k in (0, mid - 1, mid, top):
            at = n_chunks
        elif k in (mid - 2, mid + 1):
            at = n_steps - 1
        elif k == top - 1:
            at = n_chunks + 5 * LEAD
        else:
            at = 0
        when_local = when_local + jnp.where(s == k, at, 0)

    def active(j):
        return (j >= 0) & (j < n_chunks)

    def step(i, carry):
        @pl.when(i == when_local)
        def _():
            local_part()

        def rows_at(j):
            return pl.ds(pl.multiple_of(j * CHUNK, CHUNK), CHUNK)

        j_up = i - lag_up

        @pl.when(active(j_up))
        def _():
            @pl.when(up_recv)
            def _():
                up_copy(j_up).wait_recv()

            @pl.when(up_send)
            def _():
                us_ref[j_up, 0] = (a_step * ur_ref[j_up, 0].astype(F32) + lf_ref[rows_at(j_up), :]).astype(BF16)
                us_ref[j_up, 1] = (ur_ref[j_up, 1].astype(F32) + cb_ref[rows_at(j_up), :]).astype(BF16)
                up_copy(j_up).start()

        j_ca = i - lag_carry

        @pl.when(active(j_ca) & (carry_recv | carry_send))
        def _():
            @pl.when(carry_recv)
            def _():
                carry_copy(j_ca).wait_recv()

            @pl.when(carry_pass)
            def _():
                carry_copy(j_ca, cr_ref).start()

            @pl.when(carry_send)
            def _():
                cs_ref[j_ca, 0] = (cr_ref[j_ca, 0].astype(F32) + carry_w * lb_ref[rows_at(j_ca), :]).astype(BF16)
                cs_ref[j_ca, 1] = (cr_ref[j_ca, 1].astype(F32) + cf_ref[rows_at(j_ca), :]).astype(BF16)
                carry_copy(j_ca).start()

        j_dn = i - lag_down

        @pl.when(active(j_dn) & (down_recv | down_send))
        def _():
            @pl.when(down_recv)
            def _():
                down_copy(j_dn).wait_recv()

            @pl.when(down_send)
            def _():
                ds_ref[j_dn, 0] = (b_step * dr_ref[j_dn, 0].astype(F32) + lb_ref[rows_at(j_dn), :]).astype(BF16)
                ds_ref[j_dn, 1] = (dr_ref[j_dn, 1].astype(F32) + cf_ref[rows_at(j_dn), :]).astype(BF16)
                down_copy(j_dn).start()

        j_be = i - lag_below

        @pl.when(active(j_be) & (below_recv | below_send))
        def _():
            @pl.when(below_recv)
            def _():
                below_copy(j_be).wait_recv()

            @pl.when(below_send)
            def _():
                bs_ref[j_be, 0] = (b_step * br_ref[j_be, 0].astype(F32) + lb_ref[rows_at(j_be), :]).astype(BF16)
                bs_ref[j_be, 1] = (br_ref[j_be, 1].astype(F32) + cf_ref[rows_at(j_be), :]).astype(BF16)
                below_copy(j_be).start()

        return carry

    lax.fori_loop(0, n_steps, step, 0)

    ca = scalar_exp(neg_a * (span * sf))
    cbk = scalar_exp(neg_b * (span * (n_sp - 1.0 - sf)))
    low_w = scalar_exp(neg_b * (span * jnp.maximum(mid - 1.0 - sf, 0.0)))

    @pl.when(s >= low)
    def _():
        fin_ref[0] = dr_ref[:, 0].reshape(dk, dv).astype(F32)
        fin_ref[1] = dr_ref[:, 1].reshape(dk, dv).astype(F32)

    @pl.when(s < low)
    def _():
        fin_ref[0] = br_ref[:, 0].reshape(dk, dv).astype(F32) + low_w * cr_ref[:, 0].reshape(dk, dv).astype(F32)
        fin_ref[1] = br_ref[:, 1].reshape(dk, dv).astype(F32) + cr_ref[:, 1].reshape(dk, dv).astype(F32)

    s_fwd = ur_ref[:, 0].reshape(dk, dv).astype(F32) + ca * (fin_ref[1] + cf_ref[...])
    s_bwd = fin_ref[0] + cbk * (ur_ref[:, 1].reshape(dk, dv).astype(F32) + cb_ref[...])
    query = q_ref[...]
    ret = (
        ret_ref[...]
        + dot(query, s_fwd.astype(BF16)) * jnp.exp(neg_a * (place + 1.0))
        + dot(query, s_bwd.astype(BF16)) * jnp.exp(neg_b * (span - place))
    )
    centre = jnp.mean(ret, axis=-1, keepdims=True)
    ret = ret - centre
    variance = jnp.mean(ret * ret, axis=-1, keepdims=True)
    gated = (gp_ref[...] * (ret * lax.rsqrt(variance + norm_eps))).astype(BF16)
    g_ref[...] = gated.reshape(n_tp, rows, dv)

    l_wo.wait()

    def rows_of(core):
        return jnp.concatenate([g_ref[2 * k + core] for k in range(n_x)], axis=0)

    def pair_copy():
        return pltpu.make_async_remote_copy(
            src_ref=osend_ref,
            dst_ref=orecv_ref,
            send_sem=osend_sem,
            recv_sem=orecv_sem,
            device_id={"tp": partner},
            device_id_type=MESH,
        )

    osend_ref[...] = dot(rows_of(1 - c), wo_ref[...]).astype(BF16).reshape(n_x, rows, D)
    pair_copy().start()
    own_ref[...] = dot(rows_of(c), wo_ref[...]).reshape(n_x, rows, D)
    pair_copy().wait_recv()

    def out_copy(d):
        return pltpu.make_async_remote_copy(
            src_ref=xsend_ref.at[d - 1],
            dst_ref=xrecv_ref.at[d - 1],
            send_sem=rsend_sem.at[d - 1],
            recv_sem=rrecv_sem.at[d - 1],
            device_id={"tp": ((x + d) % n_x) * 2 + c},
            device_id_type=MESH,
        )

    for d in hops:
        to = (x + d) % n_x
        xsend_ref[d - 1] = (own_ref[to] + orecv_ref[to].astype(F32)).astype(BF16)
        out_copy(d).start()
    acc = own_ref[x] + orecv_ref[x].astype(F32)

    for d in range(1, n_tp):
        tpg_copy(n_tp - d, (t + d) % n_tp).wait_recv()
    gate = jnp.concatenate([gatef_ref[k] for k in range(n_tp)], axis=1)

    for d in hops:
        out_copy(d).wait_recv()
        acc = acc + xrecv_ref[d - 1].astype(F32)
    out_ref[...] = (x_ref[t].astype(F32) + gate * acc).astype(BF16)

    for d in range(1, n_sp):
        sp_copy(d).wait_send()
        spg_copy(d).wait_send()
    for d in range(1, n_tp):
        tp_copy(d, t).wait_send()
        tpg_copy(d, t).wait_send()
    lat_copy(t, partner, 0).wait_send()
    for d in range(1, n_x):
        lat_copy(t, partner, d).wait_send()
        lat_copy(t, partner, n_x + d).wait_send()
        out_copy(d).wait_send()
    pair_copy().wait_send()

    def all_sent(cond, send, sem):
        @pl.when(cond)
        def _():
            pltpu.make_async_copy(send, send, sem).wait()

    all_sent(up_send, us_ref, ussem)
    all_sent(down_send, ds_ref, dssem)
    all_sent(below_send, bs_ref, bssem)
    all_sent(carry_send | carry_pass, cs_ref, cssem)


def body(
    n_sp,
    n_tp,
    latent,
    cond,
    context,
    context_cond,
    norm_gain,
    mod_shift,
    mod_scale,
    mod_gate,
    w_query,
    w_key,
    w_value,
    w_gate,
    w_out,
    decay_rate,
    context_gain,
):
    rows, D = latent.shape
    span = rows * n_tp
    ctx_rows = context.shape[0]
    dk, dv = w_key.shape[1], w_value.shape[1]
    cols = D // n_tp
    n_x = n_tp // 2
    n_chunks = dk // CHUNK
    tab = jnp.asarray(rope_tables(span * n_sp // GRID_W, dk // 4))
    any_spec = pl.BlockSpec(memory_space=pl.ANY)
    smem = pl.BlockSpec(memory_space=pltpu.SMEM)
    dma = pltpu.SemaphoreType.DMA
    vm = pltpu.VMEM
    scratch = [
        vm((n_tp, rows, D), BF16),
        vm((ctx_rows, D), BF16),
        vm((1, cond.shape[0]), BF16),
        vm((1, cond.shape[0]), BF16),
        vm((D // LANES, LANES), BF16),
        vm(mod_shift.shape, BF16),
        vm(mod_scale.shape, BF16),
        vm(mod_gate.shape, BF16),
        vm(w_query.shape, BF16),
        vm(w_key.shape, BF16),
        vm(w_value.shape, BF16),
        vm(w_gate.shape, BF16),
        vm(w_out.shape, BF16),
        vm(tab.shape, F32),
        vm((4, cols), F32),
        vm((1, cols), F32),
        vm((n_sp - 1, 4, cols), F32),
        vm((n_sp - 1, 1, cols), F32),
        vm((n_tp, 4, cols), F32),
        vm((n_tp, 1, cols), F32),
        vm((span + ctx_rows, LANES), F32),
        vm((span + ctx_rows, D), BF16),
        vm((span, dk), BF16),
        vm((span, dv), BF16),
        vm((dk, dv), F32),
        vm((dk, dv), F32),
        vm((dk, dv), F32),
        vm((dk, dv), F32),
        vm((n_chunks, 2, CHUNK, dv), BF16),
        vm((n_chunks, 2, CHUNK, dv), BF16),
        vm((n_chunks, 2, CHUNK, dv), BF16),
        vm((n_chunks, 2, CHUNK, dv), BF16),
        vm((n_chunks, 2, CHUNK, dv), BF16),
        vm((n_chunks, 2, CHUNK, dv), BF16),
        vm((n_chunks, 2, CHUNK, dv), BF16),
        vm((n_chunks, 2, CHUNK, dv), BF16),
        vm((2, dk, dv), F32),
        vm((span, dk), BF16),
        vm((span, dv), F32),
        vm((span, dv), F32),
        vm((n_tp, rows, dv), BF16),
        vm((n_x, rows, D), BF16),
        vm((n_x, rows, D), BF16),
        vm((n_x, rows, D), F32),
        vm((n_x - 1, rows, D), BF16),
        vm((n_x - 1, rows, D), BF16),
        dma((14,)),
        dma((n_sp - 1,)),
        dma((n_sp - 1,)),
        dma((n_sp - 1,)),
        dma((n_sp - 1,)),
        dma((n_tp - 1,)),
        dma((n_tp,)),
        dma((n_tp - 1,)),
        dma((n_tp,)),
        dma((2 * n_x,)),
        dma((n_tp,)),
        dma,
        dma((n_chunks,)),
        dma,
        dma((n_chunks,)),
        dma,
        dma((n_chunks,)),
        dma,
        dma((n_chunks,)),
        dma,
        dma,
        dma((n_x - 1,)),
        dma((n_x - 1,)),
    ]
    return pl.pallas_call(
        functools.partial(kernel, n_sp, n_tp),
        out_shape=jax.ShapeDtypeStruct(latent.shape, BF16),
        in_specs=[smem, smem] + [any_spec] * 14,
        out_specs=pl.BlockSpec(memory_space=pltpu.VMEM),
        scratch_shapes=scratch,
        compiler_params=pltpu.CompilerParams(
            collective_id=0, has_side_effects=True, vmem_limit_bytes=60 * 1024 * 1024
        ),
        name="layer",
    )(
        decay_rate.reshape(2),
        context_gain,
        latent,
        cond.reshape(1, -1),
        context_cond.reshape(1, -1),
        context,
        norm_gain.reshape(D // LANES, LANES),
        mod_shift,
        mod_scale,
        mod_gate,
        w_query,
        w_key,
        w_value,
        w_gate,
        w_out,
        tab,
    )


def solution(mesh):
    return jax.shard_map(
        functools.partial(body, mesh.shape["sp"], mesh.shape["tp"]),
        mesh=mesh,
        in_specs=(
            P(("grp", "sp", "tp"), None),
            P(("grp", "sp")),
            P(("grp", "sp"), None),
            P("sp"),
            P(),
            P("sp", "tp"),
            P("sp", "tp"),
            P("sp", "tp"),
            P(None, "tp"),
            P(None, "tp"),
            P(None, "tp"),
            P(None, "tp"),
            P("tp", None),
            P(None, "tp"),
            P("tp"),
        ),
        out_specs=P(("grp", "sp", "tp"), None),
        check_vma=False,
    )
```
